32 devices in a mesh: sp: 4 (over y, x), tp: 8 (over z, core).
Axes of the slice: x: 2, y: 2, z: 4, core: 2. Of those that a mesh axis runs over, the one named last changes fastest.
Arguments:
- queries: bfloat16 [4096, 2048], P('sp', 'tp'), may hold values from -160 to 160
- key_heads: bfloat16 [4096, 512], P('sp'), may hold values from -8 to 8
- value_heads: bfloat16 [4096, 512], P('sp'), may hold values from -4 to 4
- sink_logit: float32 [16], P('tp'), may hold values from -2 to 7
- out_weight: bfloat16 [2048, 2048], P('tp'), may hold values from -0.125 to 0.125
- residual: bfloat16 [4096, 2048], P(('sp', 'tp')), may hold values from -6 to 6
- mixer_gain: float32 [2048], replicated, may hold values from 0.1 to 1.9
- expert_gain: float32 [2048], replicated, may hold values from 0.1 to 1.9
- route_group: int32 [4096], P(('sp', 'tp')), may hold values from 0 to 3, as said below
- route_member: int32 [4096, 2], P(('sp', 'tp')), may hold values from 0 to 2, as said below
- route_weight: bfloat16 [4096, 2], P(('sp', 'tp')), may hold values from 0.19921875 to 1
- gate_weight: bfloat16 [12, 2048, 2048], P('sp', None, 'tp'), may hold values from -0.125 to 0.125
- up_weight: bfloat16 [12, 2048, 2048], P('sp', None, 'tp'), may hold values from -0.125 to 0.125
- down_weight: bfloat16 [12, 2048, 2048], P('sp', 'tp'), may hold values from -0.125 to 0.125
Outputs:
- output: bfloat16 [4096, 2048], P(('sp', 'tp'))
The draws below stay inside these ranges and needn't reach their ends.
Inputs may be any that keep to these rules, and one draw needn't show every extreme that they name: `route_group`: among the tokens of one device, at most 40 name one group; in every draw one group is named by exactly 40 tokens of every device. `route_member`: the two entries of a token are different members of its group.
All inputs are finite; a program needn't handle non-finite values.
Results may differ from the reference program's by a relative error of at most 0.018.
Values may be sent and summed in bfloat16 or wider, within the bound.
A program may use at most 128 MiB of HBM per device.

```python
import jax
import jax.numpy as jnp
from jax import lax

D = 2048
HEADS = 16
KV_HEADS = 4
HEAD_DIM = 128
WINDOW = 128
BLOCK = 128
EXP_HID = 2048
GROUP_EXPERTS = 3
TOP = 2
TOK_DEV = 128
TOKENS = 4096
GROUPS = 4
EXPERTS = 12
GROUP_CAP = 40
N_TP = 8


def draw_key_heads(key, part):
    return jnp.clip(jax.random.normal(jax.random.fold_in(key, 37), (TOKENS, KV_HEADS * HEAD_DIM), jnp.float32), -4.0, 4.0).astype(jnp.bfloat16)


def draw_queries(key, part):
    drawn_rows = jnp.clip(jax.random.normal(jax.random.fold_in(key, 41), (TOKENS, HEADS * HEAD_DIM), jnp.float32), -4.0, 4.0)
    return drawn_rows.astype(jnp.bfloat16)


def route_table(key):
    base_key = jax.random.fold_in(key, 53)
    blocks = TOKENS // TOK_DEV
    slot_count = GROUPS * GROUP_CAP
    favored = jax.random.randint(jax.random.fold_in(base_key, 1), (), 0, GROUPS)

    def one_block(block_key):
        slot_order = jax.random.permutation(jax.random.fold_in(block_key, 1), slot_count)
        ranking = jnp.where(slot_order // GROUP_CAP == favored, 0, 1) * slot_count + jnp.arange(slot_count, dtype=jnp.int32)
        taken_slots = slot_order[jnp.argsort(ranking)][:TOK_DEV]
        shuffled = taken_slots[jax.random.permutation(jax.random.fold_in(block_key, 2), TOK_DEV)]
        chosen = shuffled // GROUP_CAP
        first_member = jax.random.randint(jax.random.fold_in(block_key, 3), (TOK_DEV,), 0, GROUP_EXPERTS)
        stepping = jax.random.randint(jax.random.fold_in(block_key, 4), (TOK_DEV,), 1, GROUP_EXPERTS)
        second = (first_member + stepping) % GROUP_EXPERTS
        return (chosen, jnp.stack([first_member, second], axis=1))
    block_keys = jax.random.split(jax.random.fold_in(base_key, 2), blocks)
    chosen, members = jax.vmap(one_block)(block_keys)
    return (chosen.reshape(TOKENS).astype(jnp.int32), members.reshape(TOKENS, TOP).astype(jnp.int32))


def draw_route_group(key, part):
    return route_table(key)[0]


def draw_route_member(key, part):
    return route_table(key)[1]


def block_scale(key, extent, pieces, smallest, top_value):
    def one(axis_at, shards_of):
        draws = jax.random.uniform(jax.random.fold_in(jax.random.fold_in(key, 6), axis_at), (shards_of,), jnp.float32, smallest / len(pieces), top_value / len(pieces))
        return jnp.repeat(jnp.exp(draws), extent[axis_at] // shards_of).reshape((-1,) + (1,) * (len(extent) - axis_at - 1))

    gain = one(*pieces[0])
    for cut in pieces[1:]:
        gain = gain * one(*cut)
    return gain


def noise(stream_key, extent, scale, most, cuts=(), kind=jnp.bfloat16):
    values = jax.random.normal(stream_key, extent, jnp.float32) * scale
    if len(cuts) > 0:
        values = block_scale(stream_key, extent, cuts, -0.22, 0.18) * values
    return jnp.clip(values, min=-most, max=most).astype(kind)


def setup_inputs(seed: int = 0) -> dict:
    arg_keys = jax.random.split(jax.random.key(seed), 15)
    return {
        "queries": draw_queries(jax.random.fold_in(arg_keys[14], 71), 0),
        "key_heads": draw_key_heads(jax.random.fold_in(arg_keys[14], 71), 0),
        "value_heads": noise(arg_keys[2], (TOKENS, KV_HEADS * HEAD_DIM), 1.0, 4.0, ((0, 4),)),
        "sink_logit": jnp.clip(-2.0 + 9.0 * jax.random.uniform(arg_keys[3], (HEADS,), jnp.float32) ** block_scale(arg_keys[3], (HEADS,), ((0, 8),), -0.2, 0.2), -2.0, 7.0),
        "out_weight": noise(arg_keys[4], (HEADS * HEAD_DIM, D), (HEADS * HEAD_DIM) ** -0.5, 0.125, ((0, 8),)),
        "residual": noise(arg_keys[5], (TOKENS, D), 1.0, 6.0, ((0, 32),)),
        "mixer_gain": jnp.clip(1.0 + 0.18 * jax.random.normal(arg_keys[6], (D,), jnp.float32), 0.1, 1.9),
        "expert_gain": jnp.clip(1.0 + 0.18 * jax.random.normal(arg_keys[7], (D,), jnp.float32), 0.1, 1.9),
        "route_group": draw_route_group(jax.random.fold_in(arg_keys[14], 71), 0),
        "route_member": draw_route_member(jax.random.fold_in(arg_keys[14], 71), 0),
        "route_weight": jnp.clip(0.19921875 + 0.80078125 * jax.random.uniform(arg_keys[10], (TOKENS, TOP), jnp.float32) ** block_scale(arg_keys[10], (TOKENS, TOP), ((0, 32),), -0.2, 0.2), 0.19921875, 1.0).astype(jnp.bfloat16),
        "gate_weight": noise(arg_keys[11], (EXPERTS, D, EXP_HID), D ** -0.5, 0.125, ((0, 4), (2, 8))),
        "up_weight": noise(arg_keys[12], (EXPERTS, D, EXP_HID), D ** -0.5, 0.125, ((0, 4), (2, 8))),
        "down_weight": noise(arg_keys[13], (EXPERTS, EXP_HID, D), EXP_HID ** -0.5, 0.125, ((0, 4), (1, 8))),
    }


EPS = 1e-06
NEG_BIG = -1e+30

def head_attention(queries, key_heads, value_heads, sink_logit):
    blocks = TOKENS // BLOCK
    span_rows = BLOCK + 2 * WINDOW
    key_group = HEADS // KV_HEADS
    query_pos = jnp.arange(TOKENS, dtype=jnp.int32).reshape(blocks, BLOCK)
    key_pos = (jnp.arange(blocks, dtype=jnp.int32) * BLOCK)[:, None] + jnp.arange(span_rows, dtype=jnp.int32)[None, :] - WINDOW
    inside = (jnp.abs(query_pos[:, :, None] - key_pos[:, None, :]) <= WINDOW) & (key_pos >= 0)[:, None, :] & (key_pos < TOKENS)[:, None, :]
    gather_at = jnp.clip(key_pos, 0, TOKENS - 1)

    def one_head(head_index):
        query_cols = lax.dynamic_slice_in_dim(queries, head_index * HEAD_DIM, HEAD_DIM, 1).reshape(blocks, BLOCK, HEAD_DIM)
        kv_start = head_index // key_group * HEAD_DIM
        key_cols = lax.dynamic_slice_in_dim(key_heads, kv_start, HEAD_DIM, 1)[gather_at]
        value_cols = lax.dynamic_slice_in_dim(value_heads, kv_start, HEAD_DIM, 1)[gather_at]
        scores = jnp.einsum('nqd,nkd->nqk', query_cols.astype(jnp.float32), key_cols.astype(jnp.float32)) * HEAD_DIM ** (-0.5)
        scores = jnp.where(inside, scores, NEG_BIG)
        sink_value = sink_logit[head_index].astype(jnp.float32)
        row_top = jnp.maximum(lax.optimization_barrier(jnp.max(scores, axis=2, keepdims=True)), sink_value)
        exp_terms = jnp.exp(scores - row_top)
        row_mass = lax.optimization_barrier(jnp.sum(exp_terms, axis=2, keepdims=True)) + jnp.exp(sink_value - row_top)
        weight = (exp_terms / row_mass).astype(jnp.bfloat16)
        result = jnp.einsum('nqk,nkd->nqd', weight.astype(jnp.float32), value_cols.astype(jnp.float32)).astype(jnp.bfloat16)
        return result.reshape(TOKENS, HEAD_DIM)
    per_head = lax.map(one_head, jnp.arange(HEADS, dtype=jnp.int32))
    return jnp.transpose(per_head, (1, 0, 2)).reshape(TOKENS, HEADS * HEAD_DIM)

def merge_heads(attended, out_weight):
    width = HEADS // N_TP * HEAD_DIM

    def add_block(block_index, running):
        columns = lax.dynamic_slice_in_dim(attended, block_index * width, width, 1)
        weight_rows = lax.dynamic_slice_in_dim(out_weight, block_index * width, width, 0)
        product = jnp.dot(columns, weight_rows, preferred_element_type=jnp.float32).astype(jnp.bfloat16)
        product = lax.optimization_barrier(product)
        return running + product.astype(jnp.float32)
    return lax.fori_loop(0, N_TP, add_block, jnp.zeros((TOKENS, D), jnp.float32))

def reference(queries, key_heads, value_heads, sink_logit, out_weight, residual, mixer_gain, expert_gain, route_group, route_member, route_weight, gate_weight, up_weight, down_weight):
    attended = head_attention(queries, key_heads, value_heads, sink_logit)
    projected = merge_heads(attended, out_weight)
    proj_scale = lax.rsqrt(lax.optimization_barrier(jnp.mean(projected * projected, axis=1, keepdims=True)) + EPS)
    mixed_rows = (residual.astype(jnp.float32) + mixer_gain.astype(jnp.float32) * (projected * proj_scale)).astype(jnp.bfloat16)
    mixed_float = mixed_rows.astype(jnp.float32)
    norm_scale = lax.rsqrt(lax.optimization_barrier(jnp.mean(mixed_float * mixed_float, axis=1, keepdims=True)) + EPS)
    normed = (mixed_float * norm_scale * expert_gain.astype(jnp.float32)).astype(jnp.bfloat16)
    blocks = TOKENS // TOK_DEV
    slots = blocks * GROUP_CAP
    grouped = route_group.reshape(blocks, TOK_DEV)
    chosen = (grouped[:, :, None] == jnp.arange(GROUPS, dtype=jnp.int32)[None, None, :]).astype(jnp.int32)
    group_rank = lax.optimization_barrier(jnp.sum(chosen * (jnp.cumsum(chosen, axis=1) - 1), axis=2))
    block_ids = jnp.arange(blocks, dtype=jnp.int32)[:, None]
    dest = (grouped * slots + block_ids * GROUP_CAP + group_rank).reshape(TOKENS).astype(jnp.int32)
    member_ids = jnp.arange(GROUP_EXPERTS, dtype=jnp.int32)
    token_gates = lax.optimization_barrier(jnp.sum(route_weight.astype(jnp.float32)[:, :, None] * (route_member[:, :, None] == member_ids[None, None, :]).astype(jnp.float32), axis=1))
    slot_rows = jnp.zeros((GROUPS * slots, D), jnp.bfloat16).at[dest].set(normed)
    slot_gates = jnp.zeros((GROUPS * slots, GROUP_EXPERTS), jnp.float32).at[dest].set(token_gates)
    hid_dev = EXP_HID // N_TP

    def group_experts(operands):
        rows_in, gates_in, gate_w, up_w, down_w = operands
        gate_pre = jnp.einsum('md,edh->meh', rows_in.astype(jnp.float32), gate_w.astype(jnp.float32))
        up_pre = jnp.einsum('md,edh->meh', rows_in.astype(jnp.float32), up_w.astype(jnp.float32))
        hidden = (jax.nn.silu(gate_pre) * up_pre * gates_in[:, :, None]).astype(jnp.bfloat16)
        hidden = hidden.reshape(slots, GROUP_EXPERTS, N_TP, hid_dev)
        down_blocks = down_w.reshape(GROUP_EXPERTS, N_TP, hid_dev, D)
        parts = jnp.einsum('mejh,ejhd->mjd', hidden.astype(jnp.float32), down_blocks.astype(jnp.float32))
        parts = lax.optimization_barrier(parts.astype(jnp.bfloat16))
        return lax.optimization_barrier(jnp.sum(parts.astype(jnp.float32), axis=1)).astype(jnp.bfloat16)
    group_out = lax.map(group_experts, (slot_rows.reshape(GROUPS, slots, D), slot_gates.reshape(GROUPS, slots, GROUP_EXPERTS), gate_weight.reshape(GROUPS, GROUP_EXPERTS, D, EXP_HID), up_weight.reshape(GROUPS, GROUP_EXPERTS, D, EXP_HID), down_weight.reshape(GROUPS, GROUP_EXPERTS, EXP_HID, D)))
    expert_out = group_out.reshape(GROUPS * slots, D)[dest]
    return (mixed_float + expert_out.astype(jnp.float32)).astype(jnp.bfloat16)
```

```python
import functools

import jax
import jax.numpy as jnp
from jax import lax
from jax.experimental import pallas as pl
from jax.experimental.pallas import tpu as pltpu
from jax.sharding import PartitionSpec as P

HEADS = 16
KV_HEADS = 4
HEAD_DIM = 128
WINDOW = 128
BLOCK = 128
GROUP_EXPERTS = 3


EPS = 1e-06
NEG_BIG = -1e30


def extended(block, sides, width):
    for axis, dim in sides:
        count = lax.axis_size(axis)
        forward = [(i, i + 1) for i in range(count - 1)]
        backward = [(target, source) for source, target in forward]
        low = lax.ppermute(
            lax.slice_in_dim(block, block.shape[dim] - width, None, axis=dim), axis, forward
        )
        high = lax.ppermute(lax.slice_in_dim(block, 0, width, axis=dim), axis, backward)
        block = jnp.concatenate([low, block, high], axis=dim)
    return block


def window_attention(queries, key_heads, value_heads, sink_logit):
    seq_rows = queries.shape[0]
    heads_dev = sink_logit.shape[0]
    key_group = HEADS // KV_HEADS
    key_start = lax.axis_index("tp") * heads_dev // key_group * HEAD_DIM
    key_own = lax.dynamic_slice_in_dim(key_heads, key_start, HEAD_DIM, 1)
    value_own = lax.dynamic_slice_in_dim(value_heads, key_start, HEAD_DIM, 1)
    padded = extended(jnp.stack([key_own, value_own]), (("sp", 1),), WINDOW)
    blocks = seq_rows // BLOCK
    extent = WINDOW // BLOCK
    tile_rows = padded.reshape(2, blocks + 2 * extent, BLOCK, HEAD_DIM)
    key_spans = jnp.concatenate(
        [tile_rows[:, shifted : shifted + blocks] for shifted in range(2 * extent + 1)], axis=2
    )
    offset = lax.axis_index("sp") * seq_rows
    seq_total = seq_rows * lax.axis_size("sp")
    query_pos = offset + jnp.arange(seq_rows, dtype=jnp.int32).reshape(blocks, BLOCK)
    key_pos = (
        offset
        + (jnp.arange(blocks, dtype=jnp.int32) * BLOCK)[:, None]
        + jnp.arange(BLOCK + 2 * WINDOW, dtype=jnp.int32)[None, :]
        - WINDOW
    )
    inside = (
        (jnp.abs(query_pos[:, :, None] - key_pos[:, None, :]) <= WINDOW)
        & (key_pos >= 0)[:, None, :]
        & (key_pos < seq_total)[:, None, :]
    )
    query_blocks = queries.reshape(blocks, BLOCK, heads_dev, HEAD_DIM)
    scores = jnp.einsum(
        "nqhd,nkd->nhqk", query_blocks, key_spans[0], preferred_element_type=jnp.float32
    ) * HEAD_DIM ** (-0.5)
    scores = jnp.where(inside[:, None], scores, NEG_BIG)
    sink_col = sink_logit[None, :, None, None]
    row_top = jnp.maximum(jnp.max(scores, axis=3, keepdims=True), sink_col)
    exp_terms = jnp.exp(scores - row_top)
    row_mass = jnp.sum(exp_terms, axis=3, keepdims=True) + jnp.exp(sink_col - row_top)
    weight = (exp_terms / row_mass).astype(jnp.bfloat16)
    attended = jnp.einsum(
        "nhqk,nkd->nqhd", weight, key_spans[1], preferred_element_type=jnp.float32
    ).astype(jnp.bfloat16)
    return attended.reshape(seq_rows, heads_dev * HEAD_DIM)


CORES = 2
LANES = 128
VMEM_SPEC = pl.BlockSpec(memory_space=pltpu.VMEM)


def places():
    count = lax.axis_size("tp") // CORES
    me = lax.axis_index("tp")
    chip, core = me // CORES, lax.rem(me, CORES)
    up = lax.rem(chip + 1, count) * CORES + core
    down = lax.rem(chip + count - 1, count) * CORES + core
    partner = chip * CORES + 1 - core
    return count, chip, core, (up, down), partner


def greet(neighbours, partner, peers):
    barrier = pltpu.get_barrier_semaphore()
    for target in (*neighbours, partner):
        pl.semaphore_signal(barrier, inc=1, device_id={"tp": target})
    for peer in peers:
        pl.semaphore_signal(barrier, inc=1, device_id={"sp": peer})
    pl.semaphore_wait(barrier, 3 + len(peers))


def column_halves(width):
    low = (width // LANES + 1) // 2 * LANES
    return (pl.ds(0, low), pl.ds(low, width - low)), (low, width - low)


def spread_kernel(send_ref, out_ref, own_sem, swap_send, swap_recv, ring_send, ring_recv, core_send, core_recv):
    count, chip, core, neighbours, partner = places()
    me = lax.axis_index("tp")
    groups = lax.axis_size("sp")
    group = lax.axis_index("sp")
    order = [lax.rem(group + j, groups) for j in range(groups)]
    greet(neighbours, partner, order[1:])
    halves, _ = column_halves(out_ref.shape[3])

    def swap(j):
        return pltpu.make_async_remote_copy(
            src_ref=send_ref.at[order[j]],
            dst_ref=out_ref.at[me, group],
            send_sem=swap_send.at[j],
            recv_sem=swap_recv.at[j],
            device_id={"sp": order[j]},
        )

    def ring(side, step, j, source):
        place = out_ref.at[source, order[j], :, halves[side]]
        return pltpu.make_async_remote_copy(
            src_ref=place,
            dst_ref=place,
            send_sem=ring_send.at[side, step, j],
            recv_sem=ring_recv.at[side, step, j],
            device_id={"tp": neighbours[side]},
        )

    def across(side, step, j, source):
        place = out_ref.at[source, order[j], :, halves[side]]
        return pltpu.make_async_remote_copy(
            src_ref=place,
            dst_ref=place,
            send_sem=core_send.at[side, step, j],
            recv_sem=core_recv.at[side, step, j],
            device_id={"tp": partner},
        )

    def origin(side, step):
        shift = step if side == 1 else count - step
        return lax.rem(chip + shift, count) * CORES + core

    own = pltpu.make_async_copy(send_ref.at[group], out_ref.at[me, group], own_sem)
    own.start()
    for j in range(1, groups):
        swap(j).start()
    arrival = [0] + [groups - j for j in range(1, groups)]
    for j in range(groups):
        if j == 0:
            own.wait()
        else:
            swap(arrival[j]).wait_recv()
        for side in range(2):
            ring(side, 0, j, me).start()
            across(side, 0, j, me).start()
    for step in range(1, count):
        for j in range(groups):
            for side in range(2):
                source = origin(side, step)
                ring(side, step - 1, j, source).wait_recv()
                if step < count - 1:
                    ring(side, step, j, source).start()
                across(side, step, j, source).start()
    for j in range(1, groups):
        swap(j).wait_send()
    for step in range(count):
        for j in range(groups):
            for side in range(2):
                if step < count - 1:
                    ring(side, step, j, me).wait_send()
                across(side, step, j, me).wait()


def spread(send_rows):
    groups, capacity, width = send_rows.shape
    total = lax.axis_size("tp")
    count = total // CORES
    sem = pltpu.SemaphoreType.DMA
    return pl.pallas_call(
        spread_kernel,
        out_shape=jax.ShapeDtypeStruct((total, groups, capacity, width), send_rows.dtype),
        in_specs=[VMEM_SPEC],
        out_specs=VMEM_SPEC,
        scratch_shapes=[
            sem,
            sem((groups,)),
            sem((groups,)),
            sem((2, count, groups)),
            sem((2, count, groups)),
            sem((2, count, groups)),
            sem((2, count, groups)),
        ],
        compiler_params=pltpu.CompilerParams(collective_id=1, has_side_effects=True),
        name="spread",
    )(send_rows)


def gather_sum_kernel(
    home, part_ref, out_ref, pair0, pair1, hold0, hold1, got0, got1, done,
    core_send, core_recv, ring_send, ring_recv, swap_send, swap_recv,
):
    count, chip, core, neighbours, partner = places()
    pieces = part_ref.shape[1]
    groups = lax.axis_size("sp")
    group = lax.axis_index("sp")
    if home:
        order = [lax.rem(group + j, groups) for j in range(groups)]
        order = order[1:] + order[:1]
        peers = order[:-1]
    else:
        order = list(range(pieces))
        peers = []
    greet(neighbours, partner, peers)
    halves, _ = column_halves(part_ref.shape[3])
    pair, hold, got = (pair0, pair1), (hold0, hold1), (got0, got1)

    def target(side, step):
        shift = count - 1 - step if side == 0 else 1 + step
        return lax.rem(chip + shift, count) * CORES

    def across(side, step, j):
        return pltpu.make_async_remote_copy(
            src_ref=part_ref.at[target(side, step) + 1 - core, order[j], :, halves[side]],
            dst_ref=pair[side].at[step, j],
            send_sem=core_send.at[side, step, j],
            recv_sem=core_recv.at[side, step, j],
            device_id={"tp": partner},
        )

    def ring(side, step, j):
        return pltpu.make_async_remote_copy(
            src_ref=hold[side].at[step, j],
            dst_ref=got[side].at[step, j],
            send_sem=ring_send.at[side, step, j],
            recv_sem=ring_recv.at[side, step, j],
            device_id={"tp": neighbours[side]},
        )

    def swap(j):
        return pltpu.make_async_remote_copy(
            src_ref=done.at[j],
            dst_ref=out_ref.at[group],
            send_sem=swap_send.at[j],
            recv_sem=swap_recv.at[j],
            device_id={"sp": order[j]},
        )

    for step in range(count):
        for j in range(pieces):
            for side in range(2):
                across(side, step, j).start()
    for step in range(count):
        for j in range(pieces):
            for side in range(2):
                across(side, step, j).wait_recv()
                value = part_ref[target(side, step) + core, order[j], :, halves[side]].astype(
                    jnp.float32
                ) + pair[side][step, j].astype(jnp.float32)
                if step > 0:
                    ring(side, step - 1, j).wait_recv()
                    value = value + got[side][step - 1, j].astype(jnp.float32)
                if step < count - 1:
                    hold[side][step, j] = value.astype(hold[side].dtype)
                    ring(side, step, j).start()
                elif home and j < pieces - 1:
                    done[j, :, halves[side]] = value.astype(done.dtype)
                else:
                    out_ref[order[j], :, halves[side]] = value.astype(out_ref.dtype)
            if home and step == count - 1 and j < pieces - 1:
                swap(j).start()
    for step in range(count):
        for j in range(pieces):
            for side in range(2):
                across(side, step, j).wait_send()
                if step < count - 1:
                    ring(side, step, j).wait_send()
    if home:
        for j in range(pieces - 1):
            swap(j).wait()


def gather_sum(part, home, out_type, collective_id):
    total, pieces, rows, width = part.shape
    count = total // CORES
    _, widths = column_halves(width)
    sem = pltpu.SemaphoreType.DMA
    kind = part.dtype
    return pl.pallas_call(
        functools.partial(gather_sum_kernel, home),
        out_shape=jax.ShapeDtypeStruct((pieces, rows, width), out_type),
        in_specs=[VMEM_SPEC],
        out_specs=VMEM_SPEC,
        scratch_shapes=[
            *[pltpu.VMEM((count, pieces, rows, w), kind) for w in widths],
            *[pltpu.VMEM((count, pieces, rows, w), kind) for w in widths],
            *[pltpu.VMEM((count, pieces, rows, w), kind) for w in widths],
            pltpu.VMEM((pieces, rows, width), kind),
            *[sem((2, count, pieces)) for _ in range(4)],
            sem((pieces,)),
            sem((pieces,)),
        ],
        compiler_params=pltpu.CompilerParams(
            collective_id=collective_id, has_side_effects=True
        ),
        name="home_sum" if home else "row_sum",
    )(part)


def experts_kernel(rows_ref, gate_ref, up_ref, down_ref, out_ref):
    width = out_ref.shape[1]
    rows = rows_ref[:, :width]
    gates = rows_ref[:, width:].astype(jnp.float32)
    hidden = []
    for member in range(gate_ref.shape[0]):
        gate_pre = jnp.dot(rows, gate_ref[member], preferred_element_type=jnp.float32)
        up_pre = jnp.dot(rows, up_ref[member], preferred_element_type=jnp.float32)
        value = gate_pre / (1.0 + jnp.exp(-gate_pre)) * up_pre * gates[:, member : member + 1]
        hidden.append(value.astype(jnp.bfloat16))
    out_ref[...] = jnp.dot(
        jnp.concatenate(hidden, axis=1), down_ref[...], preferred_element_type=jnp.float32
    ).astype(out_ref.dtype)


def experts(rows, gate_weight, up_weight, down_weight, block):
    total, padded = rows.shape
    members, width, hidden = gate_weight.shape
    return pl.pallas_call(
        experts_kernel,
        out_shape=jax.ShapeDtypeStruct((total, width), rows.dtype),
        grid=(total // block,),
        in_specs=[
            pl.BlockSpec((block, padded), lambda i: (i, 0)),
            pl.BlockSpec((members, width, hidden), lambda i: (0, 0, 0)),
            pl.BlockSpec((members, width, hidden), lambda i: (0, 0, 0)),
            pl.BlockSpec((members * hidden, width), lambda i: (0, 0)),
        ],
        out_specs=pl.BlockSpec((block, width), lambda i: (i, 0)),
        compiler_params=pltpu.CompilerParams(vmem_limit_bytes=48 * 1024 * 1024),
        cost_estimate=pl.CostEstimate(
            flops=6 * total * width * members * hidden,
            bytes_accessed=2 * total * (width + padded) + 6 * members * hidden * width,
            transcendentals=total * members * hidden,
        ),
        name="experts",
    )(rows, gate_weight, up_weight, down_weight.reshape(members * hidden, width))


def per_device(
    queries,
    key_heads,
    value_heads,
    sink_logit,
    out_weight,
    residual,
    mixer_gain,
    expert_gain,
    route_group,
    route_member,
    route_weight,
    gate_weight,
    up_weight,
    down_weight,
):
    attended = window_attention(queries, key_heads, value_heads, sink_logit)
    tok_rows = residual.shape[0]
    width = out_weight.shape[1]
    parts = lax.axis_size("tp")
    pieces = 4 if tok_rows % 64 == 0 else 1
    product = jnp.dot(attended, out_weight, preferred_element_type=jnp.float32).astype(jnp.bfloat16)
    projected = gather_sum(
        product.reshape(parts, pieces, tok_rows // pieces, width), False, jnp.float32, 0
    ).reshape(tok_rows, width)
    proj_scale = lax.rsqrt(jnp.mean(projected * projected, axis=1, keepdims=True) + EPS)
    mixed_rows = (residual.astype(jnp.float32) + mixer_gain * (projected * proj_scale)).astype(
        jnp.bfloat16
    )
    mixed_float = mixed_rows.astype(jnp.float32)
    norm_scale = lax.rsqrt(jnp.mean(mixed_float * mixed_float, axis=1, keepdims=True) + EPS)
    normed = (mixed_float * norm_scale * expert_gain).astype(jnp.bfloat16)
    groups = lax.axis_size("sp")
    capacity = max(2, (5 * tok_rows + 4 * groups - 1) // (4 * groups))
    group_ids = jnp.arange(groups, dtype=jnp.int32)
    chosen = (route_group[:, None] == group_ids[None, :]).astype(jnp.int32)
    group_rank = jnp.sum(chosen * (jnp.cumsum(chosen, axis=0) - 1), axis=1)
    slot_ids = route_group * capacity + group_rank
    placing = (jnp.arange(groups * capacity, dtype=jnp.int32)[:, None] == slot_ids[None, :]).astype(
        jnp.bfloat16
    )
    member_ids = jnp.arange(GROUP_EXPERTS, dtype=jnp.int32)
    token_gates = jnp.sum(
        route_weight.astype(jnp.float32)[:, :, None]
        * (route_member[:, :, None] == member_ids[None, None, :]).astype(jnp.float32),
        axis=1,
    ).astype(jnp.bfloat16)
    tail = jnp.pad(token_gates, ((0, 0), (0, LANES - GROUP_EXPERTS)))
    send_rows = (
        jnp.dot(placing, jnp.concatenate([normed, tail], axis=1), preferred_element_type=jnp.float32)
        .astype(jnp.bfloat16)
        .reshape(groups, capacity, width + LANES)
    )
    pooled = spread(send_rows)
    partial_out = experts(
        pooled.reshape(-1, width + LANES), gate_weight, up_weight, down_weight, 2 * groups * capacity
    )
    returned = gather_sum(
        partial_out.reshape(parts, groups, capacity, width), True, jnp.bfloat16, 2
    )
    expert_out = lax.dot_general(
        placing,
        returned.reshape(groups * capacity, width),
        (((0,), (0,)), ((), ())),
        preferred_element_type=jnp.float32,
    )
    return (mixed_float + expert_out).astype(jnp.bfloat16)


def solution(mesh):
    placed = (
        P("sp", "tp"),
        P("sp", None),
        P("sp", None),
        P("tp"),
        P("tp", None),
        P(("sp", "tp"), None),
        P(),
        P(),
        P(("sp", "tp")),
        P(("sp", "tp"), None),
        P(("sp", "tp"), None),
        P("sp", None, "tp"),
        P("sp", None, "tp"),
        P("sp", "tp", None),
    )
    return jax.shard_map(
        per_device, mesh=mesh, in_specs=placed, out_specs=P(("sp", "tp"), None), check_vma=False
    )
```

```python
import functools

import jax
import jax.numpy as jnp
from jax import lax
from jax.experimental import pallas as pl
from jax.experimental.pallas import tpu as pltpu
from jax.sharding import PartitionSpec as P

HEADS = 16
KV_HEADS = 4
HEAD_DIM = 128
WINDOW = 128
BLOCK = 128
GROUP_EXPERTS = 3


EPS = 1e-06
NEG_BIG = -1e30


def extended(block, sides, width):
    for axis, dim in sides:
        count = lax.axis_size(axis)
        forward = [(i, i + 1) for i in range(count - 1)]
        backward = [(target, source) for source, target in forward]
        low = lax.ppermute(
            lax.slice_in_dim(block, block.shape[dim] - width, None, axis=dim), axis, forward
        )
        high = lax.ppermute(lax.slice_in_dim(block, 0, width, axis=dim), axis, backward)
        block = jnp.concatenate([low, block, high], axis=dim)
    return block


def window_attention(queries, key_heads, value_heads, sink_logit):
    seq_rows = queries.shape[0]
    heads_dev = sink_logit.shape[0]
    key_group = HEADS // KV_HEADS
    key_start = lax.axis_index("tp") * heads_dev // key_group * HEAD_DIM
    key_own = lax.dynamic_slice_in_dim(key_heads, key_start, HEAD_DIM, 1)
    value_own = lax.dynamic_slice_in_dim(value_heads, key_start, HEAD_DIM, 1)
    padded = extended(jnp.stack([key_own, value_own]), (("sp", 1),), WINDOW)
    blocks = seq_rows // BLOCK
    extent = WINDOW // BLOCK
    tile_rows = padded.reshape(2, blocks + 2 * extent, BLOCK, HEAD_DIM)
    key_spans = jnp.concatenate(
        [tile_rows[:, shifted : shifted + blocks] for shifted in range(2 * extent + 1)], axis=2
    )
    offset = lax.axis_index("sp") * seq_rows
    seq_total = seq_rows * lax.axis_size("sp")
    query_pos = offset + jnp.arange(seq_rows, dtype=jnp.int32).reshape(blocks, BLOCK)
    key_pos = (
        offset
        + (jnp.arange(blocks, dtype=jnp.int32) * BLOCK)[:, None]
        + jnp.arange(BLOCK + 2 * WINDOW, dtype=jnp.int32)[None, :]
        - WINDOW
    )
    inside = (
        (jnp.abs(query_pos[:, :, None] - key_pos[:, None, :]) <= WINDOW)
        & (key_pos >= 0)[:, None, :]
        & (key_pos < seq_total)[:, None, :]
    )
    query_blocks = queries.reshape(blocks, BLOCK, heads_dev, HEAD_DIM)
    scores = jnp.einsum(
        "nqhd,nkd->nhqk", query_blocks, key_spans[0], preferred_element_type=jnp.float32
    ) * HEAD_DIM ** (-0.5)
    scores = jnp.where(inside[:, None], scores, NEG_BIG)
    sink_col = sink_logit[None, :, None, None]
    row_top = jnp.maximum(jnp.max(scores, axis=3, keepdims=True), sink_col)
    exp_terms = jnp.exp(scores - row_top)
    row_mass = jnp.sum(exp_terms, axis=3, keepdims=True) + jnp.exp(sink_col - row_top)
    weight = (exp_terms / row_mass).astype(jnp.bfloat16)
    attended = jnp.einsum(
        "nhqk,nkd->nqhd", weight, key_spans[1], preferred_element_type=jnp.float32
    ).astype(jnp.bfloat16)
    return attended.reshape(seq_rows, heads_dev * HEAD_DIM)


CORES = 2
LANES = 128
VMEM_SPEC = pl.BlockSpec(memory_space=pltpu.VMEM)


def places():
    count = lax.axis_size("tp") // CORES
    me = lax.axis_index("tp")
    chip, core = me // CORES, lax.rem(me, CORES)
    up = lax.rem(chip + 1, count) * CORES + core
    down = lax.rem(chip + count - 1, count) * CORES + core
    partner = chip * CORES + 1 - core
    return count, chip, core, (up, down), partner


def greet(neighbours, partner, peers):
    barrier = pltpu.get_barrier_semaphore()
    for target in (*neighbours, partner):
        pl.semaphore_signal(barrier, inc=1, device_id={"tp": target})
    for peer in peers:
        pl.semaphore_signal(barrier, inc=1, device_id={"sp": peer})
    pl.semaphore_wait(barrier, 3 + len(peers))


def spread_kernel(send_ref, out_ref, own_sem, swap_send, swap_recv, line_send, line_recv, core_send, core_recv):
    count, chip, core, neighbours, partner = places()
    me = lax.axis_index("tp")
    groups = lax.axis_size("sp")
    group = lax.axis_index("sp")
    order = [lax.rem(group + j, groups) for j in range(groups)]
    greet(neighbours, partner, order[1:])

    def swap(j):
        return pltpu.make_async_remote_copy(
            src_ref=send_ref.at[order[j]],
            dst_ref=out_ref.at[me, group],
            send_sem=swap_send.at[j],
            recv_sem=swap_recv.at[j],
            device_id={"sp": order[j]},
        )

    def line(side, step, j, source):
        place = out_ref.at[source, order[j]]
        return pltpu.make_async_remote_copy(
            src_ref=place,
            dst_ref=place,
            send_sem=line_send.at[side, step, j],
            recv_sem=line_recv.at[side, step, j],
            device_id={"tp": neighbours[side]},
        )

    def across(side, step, j, source):
        place = out_ref.at[source, order[j]]
        return pltpu.make_async_remote_copy(
            src_ref=place,
            dst_ref=place,
            send_sem=core_send.at[side, step, j],
            recv_sem=core_recv.at[side, step, j],
            device_id={"tp": partner},
        )

    def behind(side, step):
        return chip >= step if side == 0 else chip + step < count

    def origin(side, step):
        return (chip - step if side == 0 else chip + step) * CORES + core

    ahead = (chip + 1 < count, chip >= 1)
    own = pltpu.make_async_copy(send_ref.at[group], out_ref.at[me, group], own_sem)
    own.start()
    for j in range(1, groups):
        swap(j).start()
    for j in range(groups):
        if j == 0:
            own.wait()
        else:
            swap(groups - j).wait_recv()
        for side in range(2):

            @pl.when(ahead[side])
            def _():
                line(side, 0, j, me).start()

        across(0, 0, j, me).start()
    for step in range(1, count):
        for j in range(groups):
            for side in range(2):

                @pl.when(behind(side, step))
                def _():
                    source = origin(side, step)
                    line(side, step - 1, j, source).wait_recv()
                    if step < count - 1:

                        @pl.when(ahead[side])
                        def _():
                            line(side, step, j, source).start()

                    across(side, step, j, source).start()

    for j in range(1, groups):
        swap(j).wait_send()
    for j in range(groups):
        across(0, 0, j, me).wait()
    for step in range(count):
        for j in range(groups):
            for side in range(2):
                if step < count - 1:

                    @pl.when(behind(side, step) & ahead[side])
                    def _():
                        line(side, step, j, me).wait_send()

                if step > 0:

                    @pl.when(behind(side, step))
                    def _():
                        across(side, step, j, me).wait()


def spread(send_rows):
    groups, capacity, width = send_rows.shape
    total = lax.axis_size("tp")
    count = total // CORES
    sem = pltpu.SemaphoreType.DMA
    return pl.pallas_call(
        spread_kernel,
        out_shape=jax.ShapeDtypeStruct((total, groups, capacity, width), send_rows.dtype),
        in_specs=[VMEM_SPEC],
        out_specs=VMEM_SPEC,
        scratch_shapes=[
            sem,
            sem((groups,)),
            sem((groups,)),
            sem((2, count, groups)),
            sem((2, count, groups)),
            sem((2, count, groups)),
            sem((2, count, groups)),
        ],
        compiler_params=pltpu.CompilerParams(collective_id=1, has_side_effects=True),
        name="spread",
    )(send_rows)


def gather_sum_kernel(
    home, part_ref, out_ref, pair, got, done, final,
    core_send, core_recv, line_send, line_recv, swap_send, swap_recv,
):
    count, chip, core, neighbours, partner = places()
    pieces = part_ref.shape[1]
    groups = lax.axis_size("sp")
    group = lax.axis_index("sp")
    if home:
        order = [lax.rem(group + j, groups) for j in range(groups)]
        order = order[1:] + order[:1]
        peers = order[:-1]
    else:
        order = list(range(pieces))
        peers = []
    greet(neighbours, partner, peers)

    def across(dest, j):
        return pltpu.make_async_remote_copy(
            src_ref=part_ref.at[dest * CORES + 1 - core, order[j]],
            dst_ref=pair.at[dest, j],
            send_sem=core_send.at[dest, j],
            recv_sem=core_recv.at[dest, j],
            device_id={"tp": partner},
        )

    def line(side, dest, j):
        return pltpu.make_async_remote_copy(
            src_ref=pair.at[dest, j],
            dst_ref=got.at[side, dest, j],
            send_sem=line_send.at[side, dest, j],
            recv_sem=line_recv.at[side, dest, j],
            device_id={"tp": neighbours[side]},
        )

    def swap(j):
        return pltpu.make_async_remote_copy(
            src_ref=done.at[j],
            dst_ref=out_ref.at[group],
            send_sem=swap_send.at[j],
            recv_sem=swap_recv.at[j],
            device_id={"sp": order[j]},
        )

    def local(dest, j):
        across(dest, j).wait_recv()
        return part_ref[dest * CORES + core, order[j]].astype(jnp.float32) + pair[
            dest, j
        ].astype(jnp.float32)

    sends = []
    for step in range(count - 1):
        sends += [(0, count - 1 - step), (1, step)]
    first = []
    for _, dest in sends:
        if dest not in first:
            first.append(dest)
    for dest in first:
        for j in range(pieces):
            across(dest, j).start()
    start = (chip == 0, chip == count - 1)
    inside = (chip > 0, chip < count - 1)
    for step in range(count - 1):
        for j in range(pieces):
            for side, dest in sends[2 * step : 2 * step + 2]:
                toward = chip < dest if side == 0 else chip > dest

                @pl.when(start[side])
                def _():
                    pair[dest, j] = local(dest, j).astype(pair.dtype)

                @pl.when(inside[side] & toward)
                def _():
                    value = local(dest, j)
                    line(side, dest, j).wait_recv()
                    pair[dest, j] = (value + got[side, dest, j].astype(jnp.float32)).astype(
                        pair.dtype
                    )

                @pl.when(toward)
                def _():
                    line(side, dest, j).start()

    for j in range(pieces):
        final[...] = local(chip, j)
        for side in range(2):

            @pl.when(inside[side])
            def _():
                line(side, chip, j).wait_recv()
                final[...] += got[side, chip, j].astype(jnp.float32)

        if home and j < pieces - 1:
            done[j] = final[...].astype(done.dtype)
            swap(j).start()
        else:
            out_ref[order[j]] = final[...].astype(out_ref.dtype)
    for j in range(pieces):
        for dest in range(count):
            across(dest, j).wait_send()
        for side, dest in sends:

            @pl.when(chip < dest if side == 0 else chip > dest)
            def _():
                line(side, dest, j).wait_send()

    if home:
        for j in range(pieces - 1):
            swap(j).wait()


def gather_sum(part, home, out_type, collective_id):
    total, pieces, rows, width = part.shape
    count = total // CORES
    sem = pltpu.SemaphoreType.DMA
    kind = part.dtype
    return pl.pallas_call(
        functools.partial(gather_sum_kernel, home),
        out_shape=jax.ShapeDtypeStruct((pieces, rows, width), out_type),
        in_specs=[VMEM_SPEC],
        out_specs=VMEM_SPEC,
        scratch_shapes=[
            pltpu.VMEM((count, pieces, rows, width), kind),
            pltpu.VMEM((2, count, pieces, rows, width), kind),
            pltpu.VMEM((pieces, rows, width), kind),
            pltpu.VMEM((rows, width), jnp.float32),
            sem((count, pieces)),
            sem((count, pieces)),
            sem((2, count, pieces)),
            sem((2, count, pieces)),
            sem((pieces,)),
            sem((pieces,)),
        ],
        compiler_params=pltpu.CompilerParams(
            collective_id=collective_id, has_side_effects=True
        ),
        name="home_sum" if home else "row_sum",
    )(part)


def experts_kernel(rows_ref, gate_ref, up_ref, down_ref, out_ref):
    width = out_ref.shape[1]
    rows = rows_ref[:, :width]
    gates = rows_ref[:, width:].astype(jnp.float32)
    hidden = []
    for member in range(gate_ref.shape[0]):
        gate_pre = jnp.dot(rows, gate_ref[member], preferred_element_type=jnp.float32)
        up_pre = jnp.dot(rows, up_ref[member], preferred_element_type=jnp.float32)
        value = gate_pre / (1.0 + jnp.exp(-gate_pre)) * up_pre * gates[:, member : member + 1]
        hidden.append(value.astype(jnp.bfloat16))
    out_ref[...] = jnp.dot(
        jnp.concatenate(hidden, axis=1), down_ref[...], preferred_element_type=jnp.float32
    ).astype(out_ref.dtype)


def experts(rows, gate_weight, up_weight, down_weight, block):
    total, padded = rows.shape
    members, width, hidden = gate_weight.shape
    return pl.pallas_call(
        experts_kernel,
        out_shape=jax.ShapeDtypeStruct((total, width), rows.dtype),
        grid=(total // block,),
        in_specs=[
            pl.BlockSpec((block, padded), lambda i: (i, 0)),
            pl.BlockSpec((members, width, hidden), lambda i: (0, 0, 0)),
            pl.BlockSpec((members, width, hidden), lambda i: (0, 0, 0)),
            pl.BlockSpec((members * hidden, width), lambda i: (0, 0)),
        ],
        out_specs=pl.BlockSpec((block, width), lambda i: (i, 0)),
        compiler_params=pltpu.CompilerParams(vmem_limit_bytes=48 * 1024 * 1024),
        cost_estimate=pl.CostEstimate(
            flops=6 * total * width * members * hidden,
            bytes_accessed=2 * total * (width + padded) + 6 * members * hidden * width,
            transcendentals=total * members * hidden,
        ),
        name="experts",
    )(rows, gate_weight, up_weight, down_weight.reshape(members * hidden, width))


def per_device(
    queries,
    key_heads,
    value_heads,
    sink_logit,
    out_weight,
    residual,
    mixer_gain,
    expert_gain,
    route_group,
    route_member,
    route_weight,
    gate_weight,
    up_weight,
    down_weight,
):
    attended = window_attention(queries, key_heads, value_heads, sink_logit)
    tok_rows = residual.shape[0]
    width = out_weight.shape[1]
    parts = lax.axis_size("tp")
    pieces = 4 if tok_rows % 64 == 0 else 1
    product = jnp.dot(attended, out_weight, preferred_element_type=jnp.float32).astype(jnp.bfloat16)
    projected = gather_sum(
        product.reshape(parts, pieces, tok_rows // pieces, width), False, jnp.float32, 0
    ).reshape(tok_rows, width)
    proj_scale = lax.rsqrt(jnp.mean(projected * projected, axis=1, keepdims=True) + EPS)
    mixed_rows = (residual.astype(jnp.float32) + mixer_gain * (projected * proj_scale)).astype(
        jnp.bfloat16
    )
    mixed_float = mixed_rows.astype(jnp.float32)
    norm_scale = lax.rsqrt(jnp.mean(mixed_float * mixed_float, axis=1, keepdims=True) + EPS)
    normed = (mixed_float * norm_scale * expert_gain).astype(jnp.bfloat16)
    groups = lax.axis_size("sp")
    capacity = max(2, (5 * tok_rows + 4 * groups - 1) // (4 * groups))
    group_ids = jnp.arange(groups, dtype=jnp.int32)
    chosen = (route_group[:, None] == group_ids[None, :]).astype(jnp.int32)
    group_rank = jnp.sum(chosen * (jnp.cumsum(chosen, axis=0) - 1), axis=1)
    slot_ids = route_group * capacity + group_rank
    placing = (jnp.arange(groups * capacity, dtype=jnp.int32)[:, None] == slot_ids[None, :]).astype(
        jnp.bfloat16
    )
    member_ids = jnp.arange(GROUP_EXPERTS, dtype=jnp.int32)
    token_gates = jnp.sum(
        route_weight.astype(jnp.float32)[:, :, None]
        * (route_member[:, :, None] == member_ids[None, None, :]).astype(jnp.float32),
        axis=1,
    ).astype(jnp.bfloat16)
    tail = jnp.pad(token_gates, ((0, 0), (0, LANES - GROUP_EXPERTS)))
    send_rows = (
        jnp.dot(placing, jnp.concatenate([normed, tail], axis=1), preferred_element_type=jnp.float32)
        .astype(jnp.bfloat16)
        .reshape(groups, capacity, width + LANES)
    )
    pooled = spread(send_rows)
    partial_out = experts(
        pooled.reshape(-1, width + LANES), gate_weight, up_weight, down_weight, 2 * groups * capacity
    )
    returned = gather_sum(
        partial_out.reshape(parts, groups, capacity, width), True, jnp.bfloat16, 2
    )
    expert_out = lax.dot_general(
        placing,
        returned.reshape(groups * capacity, width),
        (((0,), (0,)), ((), ())),
        preferred_element_type=jnp.float32,
    )
    return (mixed_float + expert_out).astype(jnp.bfloat16)


def solution(mesh):
    placed = (
        P("sp", "tp"),
        P("sp", None),
        P("sp", None),
        P("tp"),
        P("tp", None),
        P(("sp", "tp"), None),
        P(),
        P(),
        P(("sp", "tp")),
        P(("sp", "tp"), None),
        P(("sp", "tp"), None),
        P("sp", None, "tp"),
        P("sp", None, "tp"),
        P("sp", "tp", None),
    )
    return jax.shard_map(
        per_device, mesh=mesh, in_specs=placed, out_specs=P(("sp", "tp"), None), check_vma=False
    )
```

```python
import functools

import jax
import jax.numpy as jnp
from jax import lax
from jax.experimental import pallas as pl
from jax.experimental.pallas import tpu as pltpu
from jax.sharding import PartitionSpec as P

HEADS = 16
KV_HEADS = 4
HEAD_DIM = 128
WINDOW = 128
BLOCK = 128
GROUP_EXPERTS = 3


EPS = 1e-06
NEG_BIG = -1e30


def extended(block, sides, width):
    for axis, dim in sides:
        count = lax.axis_size(axis)
        forward = [(i, i + 1) for i in range(count - 1)]
        backward = [(target, source) for source, target in forward]
        low = lax.ppermute(
            lax.slice_in_dim(block, block.shape[dim] - width, None, axis=dim), axis, forward
        )
        high = lax.ppermute(lax.slice_in_dim(block, 0, width, axis=dim), axis, backward)
        block = jnp.concatenate([low, block, high], axis=dim)
    return block


def window_attention(queries, key_heads, value_heads, sink_logit):
    seq_rows = queries.shape[0]
    heads_dev = sink_logit.shape[0]
    key_group = HEADS // KV_HEADS
    key_start = lax.axis_index("tp") * heads_dev // key_group * HEAD_DIM
    key_own = lax.dynamic_slice_in_dim(key_heads, key_start, HEAD_DIM, 1)
    value_own = lax.dynamic_slice_in_dim(value_heads, key_start, HEAD_DIM, 1)
    padded = extended(jnp.stack([key_own, value_own]), (("sp", 1),), WINDOW)
    blocks = seq_rows // BLOCK
    extent = WINDOW // BLOCK
    tile_rows = padded.reshape(2, blocks + 2 * extent, BLOCK, HEAD_DIM)
    key_spans = jnp.concatenate(
        [tile_rows[:, shifted : shifted + blocks] for shifted in range(2 * extent + 1)], axis=2
    )
    offset = lax.axis_index("sp") * seq_rows
    seq_total = seq_rows * lax.axis_size("sp")
    query_pos = offset + jnp.arange(seq_rows, dtype=jnp.int32).reshape(blocks, BLOCK)
    key_pos = (
        offset
        + (jnp.arange(blocks, dtype=jnp.int32) * BLOCK)[:, None]
        + jnp.arange(BLOCK + 2 * WINDOW, dtype=jnp.int32)[None, :]
        - WINDOW
    )
    inside = (
        (jnp.abs(query_pos[:, :, None] - key_pos[:, None, :]) <= WINDOW)
        & (key_pos >= 0)[:, None, :]
        & (key_pos < seq_total)[:, None, :]
    )
    query_blocks = queries.reshape(blocks, BLOCK, heads_dev, HEAD_DIM)
    scores = jnp.einsum(
        "nqhd,nkd->nhqk", query_blocks, key_spans[0], preferred_element_type=jnp.float32
    ) * HEAD_DIM ** (-0.5)
    scores = jnp.where(inside[:, None], scores, NEG_BIG)
    sink_col = sink_logit[None, :, None, None]
    row_top = jnp.maximum(jnp.max(scores, axis=3, keepdims=True), sink_col)
    exp_terms = jnp.exp(scores - row_top)
    row_mass = jnp.sum(exp_terms, axis=3, keepdims=True) + jnp.exp(sink_col - row_top)
    weight = (exp_terms / row_mass).astype(jnp.bfloat16)
    attended = jnp.einsum(
        "nhqk,nkd->nqhd", weight, key_spans[1], preferred_element_type=jnp.float32
    ).astype(jnp.bfloat16)
    return attended.reshape(seq_rows, heads_dev * HEAD_DIM)


CORES = 2
LANES = 128
VMEM_SPEC = pl.BlockSpec(memory_space=pltpu.VMEM)


def places():
    count = lax.axis_size("tp") // CORES
    me = lax.axis_index("tp")
    chip, core = me // CORES, lax.rem(me, CORES)
    up = lax.rem(chip + 1, count) * CORES + core
    down = lax.rem(chip + count - 1, count) * CORES + core
    partner = chip * CORES + 1 - core
    return count, chip, core, (up, down), partner


def greet(neighbours, partner, peers):
    barrier = pltpu.get_barrier_semaphore()
    for target in (*neighbours, partner):
        pl.semaphore_signal(barrier, inc=1, device_id={"tp": target})
    for peer in peers:
        pl.semaphore_signal(barrier, inc=1, device_id={"sp": peer})
    pl.semaphore_wait(barrier, 3 + len(peers))


def column_halves(width):
    low = (width // LANES + 1) // 2 * LANES
    return (pl.ds(0, low), pl.ds(low, width - low)), (low, width - low)


def spread_kernel(send_ref, out_ref, own_sem, swap_send, swap_recv, ring_send, ring_recv, core_send, core_recv):
    count, chip, core, neighbours, partner = places()
    me = lax.axis_index("tp")
    groups = lax.axis_size("sp")
    group = lax.axis_index("sp")
    order = [lax.rem(group + j, groups) for j in range(groups)]
    greet(neighbours, partner, order[1:])
    halves, _ = column_halves(out_ref.shape[3])

    def swap(j):
        return pltpu.make_async_remote_copy(
            src_ref=send_ref.at[order[j]],
            dst_ref=out_ref.at[me, group],
            send_sem=swap_send.at[j],
            recv_sem=swap_recv.at[j],
            device_id={"sp": order[j]},
        )

    def ring(side, step, j, source):
        place = out_ref.at[source, order[j], :, halves[side]]
        return pltpu.make_async_remote_copy(
            src_ref=place,
            dst_ref=place,
            send_sem=ring_send.at[side, step, j],
            recv_sem=ring_recv.at[side, step, j],
            device_id={"tp": neighbours[side]},
        )

    def across(side, step, j, source):
        place = out_ref.at[source, order[j], :, halves[side]]
        return pltpu.make_async_remote_copy(
            src_ref=place,
            dst_ref=place,
            send_sem=core_send.at[side, step, j],
            recv_sem=core_recv.at[side, step, j],
            device_id={"tp": partner},
        )

    def origin(side, step):
        shift = step if side == 1 else count - step
        return lax.rem(chip + shift, count) * CORES + core

    own = pltpu.make_async_copy(send_ref.at[group], out_ref.at[me, group], own_sem)
    own.start()
    for j in range(1, groups):
        swap(j).start()
    arrival = [0] + [groups - j for j in range(1, groups)]
    for j in range(groups):
        if j == 0:
            own.wait()
        else:
            swap(arrival[j]).wait_recv()
        for side in range(2):
            ring(side, 0, j, me).start()
            across(side, 0, j, me).start()
    for step in range(1, count):
        for j in range(groups):
            for side in range(2):
                source = origin(side, step)
                ring(side, step - 1, j, source).wait_recv()
                if step < count - 1:
                    ring(side, step, j, source).start()
                across(side, step, j, source).start()
    for j in range(1, groups):
        swap(j).wait_send()
    for step in range(count):
        for j in range(groups):
            for side in range(2):
                if step < count - 1:
                    ring(side, step, j, me).wait_send()
                across(side, step, j, me).wait()


def spread(send_rows):
    groups, capacity, width = send_rows.shape
    total = lax.axis_size("tp")
    count = total // CORES
    sem = pltpu.SemaphoreType.DMA
    return pl.pallas_call(
        spread_kernel,
        out_shape=jax.ShapeDtypeStruct((total, groups, capacity, width), send_rows.dtype),
        in_specs=[VMEM_SPEC],
        out_specs=VMEM_SPEC,
        scratch_shapes=[
            sem,
            sem((groups,)),
            sem((groups,)),
            sem((2, count, groups)),
            sem((2, count, groups)),
            sem((2, count, groups)),
            sem((2, count, groups)),
        ],
        compiler_params=pltpu.CompilerParams(collective_id=1, has_side_effects=True),
        name="spread",
    )(send_rows)


def gather_sum_kernel(
    home, part_ref, out_ref, pair0, pair1, hold0, hold1, got0, got1, done,
    core_send, core_recv, ring_send, ring_recv, swap_send, swap_recv,
):
    count, chip, core, neighbours, partner = places()
    pieces = part_ref.shape[1]
    groups = lax.axis_size("sp")
    group = lax.axis_index("sp")
    if home:
        order = [lax.rem(group + j, groups) for j in range(groups)]
        order = order[1:] + order[:1]
        peers = order[:-1]
    else:
        order = list(range(pieces))
        peers = []
    greet(neighbours, partner, peers)
    halves, _ = column_halves(part_ref.shape[3])
    pair, hold, got = (pair0, pair1), (hold0, hold1), (got0, got1)

    def target(side, step):
        shift = count - 1 - step if side == 0 else 1 + step
        return lax.rem(chip + shift, count) * CORES

    def across(side, step, j):
        return pltpu.make_async_remote_copy(
            src_ref=part_ref.at[target(side, step) + 1 - core, order[j], :, halves[side]],
            dst_ref=pair[side].at[step, j],
            send_sem=core_send.at[side, step, j],
            recv_sem=core_recv.at[side, step, j],
            device_id={"tp": partner},
        )

    def ring(side, step, j):
        return pltpu.make_async_remote_copy(
            src_ref=hold[side].at[step, j],
            dst_ref=got[side].at[step, j],
            send_sem=ring_send.at[side, step, j],
            recv_sem=ring_recv.at[side, step, j],
            device_id={"tp": neighbours[side]},
        )

    def swap(j):
        return pltpu.make_async_remote_copy(
            src_ref=done.at[j],
            dst_ref=out_ref.at[group],
            send_sem=swap_send.at[j],
            recv_sem=swap_recv.at[j],
            device_id={"sp": order[j]},
        )

    for step in range(count):
        for j in range(pieces):
            for side in range(2):
                across(side, step, j).start()
    for step in range(count):
        for j in range(pieces):
            for side in range(2):
                across(side, step, j).wait_recv()
                value = part_ref[target(side, step) + core, order[j], :, halves[side]].astype(
                    jnp.float32
                ) + pair[side][step, j].astype(jnp.float32)
                if step > 0:
                    ring(side, step - 1, j).wait_recv()
                    value = value + got[side][step - 1, j].astype(jnp.float32)
                if step < count - 1:
                    hold[side][step, j] = value.astype(hold[side].dtype)
                    ring(side, step, j).start()
                elif home and j < pieces - 1:
                    done[j, :, halves[side]] = value.astype(done.dtype)
                else:
                    out_ref[order[j], :, halves[side]] = value.astype(out_ref.dtype)
            if home and step == count - 1 and j < pieces - 1:
                swap(j).start()
    for step in range(count):
        for j in range(pieces):
            for side in range(2):
                across(side, step, j).wait_send()
                if step < count - 1:
                    ring(side, step, j).wait_send()
    if home:
        for j in range(pieces - 1):
            swap(j).wait()


def gather_sum(part, home, out_type, collective_id):
    total, pieces, rows, width = part.shape
    count = total // CORES
    _, widths = column_halves(width)
    sem = pltpu.SemaphoreType.DMA
    kind = part.dtype
    return pl.pallas_call(
        functools.partial(gather_sum_kernel, home),
        out_shape=jax.ShapeDtypeStruct((pieces, rows, width), out_type),
        in_specs=[VMEM_SPEC],
        out_specs=VMEM_SPEC,
        scratch_shapes=[
            *[pltpu.VMEM((count, pieces, rows, w), kind) for w in widths],
            *[pltpu.VMEM((count, pieces, rows, w), kind) for w in widths],
            *[pltpu.VMEM((count, pieces, rows, w), kind) for w in widths],
            pltpu.VMEM((pieces, rows, width), kind),
            *[sem((2, count, pieces)) for _ in range(4)],
            sem((pieces,)),
            sem((pieces,)),
        ],
        compiler_params=pltpu.CompilerParams(
            collective_id=collective_id, has_side_effects=True
        ),
        name="home_sum" if home else "row_sum",
    )(part)


def experts_kernel(rows_ref, gate_ref, up_ref, down_ref, out_ref):
    width = out_ref.shape[1]
    rows = rows_ref[:, :width]
    gates = rows_ref[:, width:].astype(jnp.float32)
    hidden = []
    for member in range(gate_ref.shape[0]):
        gate_pre = jnp.dot(rows, gate_ref[member], preferred_element_type=jnp.float32)
        up_pre = jnp.dot(rows, up_ref[member], preferred_element_type=jnp.float32)
        value = gate_pre / (1.0 + jnp.exp(-gate_pre)) * up_pre * gates[:, member : member + 1]
        hidden.append(value.astype(jnp.bfloat16))
    out_ref[...] = jnp.dot(
        jnp.concatenate(hidden, axis=1), down_ref[...], preferred_element_type=jnp.float32
    ).astype(out_ref.dtype)


def experts(rows, gate_weight, up_weight, down_weight, block):
    total, padded = rows.shape
    members, width, hidden = gate_weight.shape
    return pl.pallas_call(
        experts_kernel,
        out_shape=jax.ShapeDtypeStruct((total, width), rows.dtype),
        grid=(total // block,),
        in_specs=[
            pl.BlockSpec((block, padded), lambda i: (i, 0)),
            pl.BlockSpec((members, width, hidden), lambda i: (0, 0, 0)),
            pl.BlockSpec((members, width, hidden), lambda i: (0, 0, 0)),
            pl.BlockSpec((members * hidden, width), lambda i: (0, 0)),
        ],
        out_specs=pl.BlockSpec((block, width), lambda i: (i, 0)),
        compiler_params=pltpu.CompilerParams(vmem_limit_bytes=48 * 1024 * 1024),
        cost_estimate=pl.CostEstimate(
            flops=6 * total * width * members * hidden,
            bytes_accessed=2 * total * (width + padded) + 6 * members * hidden * width,
            transcendentals=total * members * hidden,
        ),
        name="experts",
    )(rows, gate_weight, up_weight, down_weight.reshape(members * hidden, width))


def per_device(
    queries,
    key_heads,
    value_heads,
    sink_logit,
    out_weight,
    residual,
    mixer_gain,
    expert_gain,
    route_group,
    route_member,
    route_weight,
    gate_weight,
    up_weight,
    down_weight,
):
    attended = window_attention(queries, key_heads, value_heads, sink_logit)
    tok_rows = residual.shape[0]
    width = out_weight.shape[1]
    parts = lax.axis_size("tp")
    pieces = 8 if tok_rows % 128 == 0 else 1
    product = jnp.dot(attended, out_weight, preferred_element_type=jnp.float32).astype(jnp.bfloat16)
    projected = gather_sum(
        product.reshape(parts, pieces, tok_rows // pieces, width), False, jnp.float32, 0
    ).reshape(tok_rows, width)
    proj_scale = lax.rsqrt(jnp.mean(projected * projected, axis=1, keepdims=True) + EPS)
    mixed_rows = (residual.astype(jnp.float32) + mixer_gain * (projected * proj_scale)).astype(
        jnp.bfloat16
    )
    mixed_float = mixed_rows.astype(jnp.float32)
    norm_scale = lax.rsqrt(jnp.mean(mixed_float * mixed_float, axis=1, keepdims=True) + EPS)
    normed = (mixed_float * norm_scale * expert_gain).astype(jnp.bfloat16)
    groups = lax.axis_size("sp")
    capacity = max(2, (5 * tok_rows + 4 * groups - 1) // (4 * groups))
    group_ids = jnp.arange(groups, dtype=jnp.int32)
    chosen = (route_group[:, None] == group_ids[None, :]).astype(jnp.int32)
    group_rank = jnp.sum(chosen * (jnp.cumsum(chosen, axis=0) - 1), axis=1)
    slot_ids = route_group * capacity + group_rank
    placing = (jnp.arange(groups * capacity, dtype=jnp.int32)[:, None] == slot_ids[None, :]).astype(
        jnp.bfloat16
    )
    member_ids = jnp.arange(GROUP_EXPERTS, dtype=jnp.int32)
    token_gates = jnp.sum(
        route_weight.astype(jnp.float32)[:, :, None]
        * (route_member[:, :, None] == member_ids[None, None, :]).astype(jnp.float32),
        axis=1,
    ).astype(jnp.bfloat16)
    tail = jnp.pad(token_gates, ((0, 0), (0, LANES - GROUP_EXPERTS)))
    send_rows = (
        jnp.dot(placing, jnp.concatenate([normed, tail], axis=1), preferred_element_type=jnp.float32)
        .astype(jnp.bfloat16)
        .reshape(groups, capacity, width + LANES)
    )
    pooled = spread(send_rows)
    partial_out = experts(
        pooled.reshape(-1, width + LANES), gate_weight, up_weight, down_weight, 2 * groups * capacity
    )
    returned = gather_sum(
        partial_out.reshape(parts, groups, capacity, width), True, jnp.bfloat16, 2
    )
    expert_out = lax.dot_general(
        placing,
        returned.reshape(groups * capacity, width),
        (((0,), (0,)), ((), ())),
        preferred_element_type=jnp.float32,
    )
    return (mixed_float + expert_out).astype(jnp.bfloat16)


def solution(mesh):
    placed = (
        P("sp", "tp"),
        P("sp", None),
        P("sp", None),
        P("tp"),
        P("tp", None),
        P(("sp", "tp"), None),
        P(),
        P(),
        P(("sp", "tp")),
        P(("sp", "tp"), None),
        P(("sp", "tp"), None),
        P("sp", None, "tp"),
        P("sp", None, "tp"),
        P("sp", "tp", None),
    )
    return jax.shard_map(
        per_device, mesh=mesh, in_specs=placed, out_specs=P(("sp", "tp"), None), check_vma=False
    )
```
